128 devices in a mesh: sp: 64 (over z, y, x), tp: 2 (over core).
Axes of the slice: x: 4, y: 4, z: 4, core: 2. Of those that a mesh axis runs over, the one named last changes fastest.
Arguments:
- moe_input: bfloat16 [16384, 2048], P('sp'), may hold values from -6 to 6
- cotangent: bfloat16 [16384, 2048], P('sp'), may hold values from -16 to 16
- expert_ids: int32 [16384, 2], P('sp'), may hold values from 0 to 63, all different within a row; in each aligned block of 256 rows (0 to 255, 256 to 511, ...) at most 16 rows name the same one
- route_weight: float32 [16384, 2], P('sp'), may hold values from 0.05 to 0.6
- gate_proj: bfloat16 [64, 2048, 1024], P('sp', None, 'tp'), may hold values from -0.125 to 0.125
- up_proj: bfloat16 [64, 2048, 1024], P('sp', None, 'tp'), may hold values from -0.125 to 0.125
- down_proj: bfloat16 [64, 1024, 2048], P('sp', 'tp'), may hold values from -0.1875 to 0.1875
- out_weight: bfloat16 [2048, 2048], P(None, 'tp'), may hold values from -0.125 to 0.125
- recur_input: bfloat16 [16384, 2048], P('sp', 'tp'), may hold values from -6 to 6
- gate_input: bfloat16 [16384, 2048], P('sp', 'tp'), may hold values from -6 to 6
- states: float32 [16384, 2048], P('sp', 'tp'), may hold values from -6 to 6
- conv_taps: bfloat16 [4, 2048], P(None, 'tp'), may hold values from -3 to 3
- decay_gate_w: bfloat16 [16, 128, 128], P('tp'), may hold values from -0.5 to 0.5
- input_gate_w: bfloat16 [16, 128, 128], P('tp'), may hold values from -0.5 to 0.5
- decay_rate: float32 [2048], P('tp'), may hold values from 1.8310547e-06 to 0.008
- decay_extra: float32 [16384, 2048], P('sp', 'tp'), may hold values from -0.77 to 0
Outputs:
- gate_proj_grad: bfloat16 [64, 2048, 1024], P('sp', None, 'tp')
- up_proj_grad: bfloat16 [64, 2048, 1024], P('sp', None, 'tp')
- down_proj_grad: bfloat16 [64, 1024, 2048], P('sp', 'tp')
- out_weight_grad: float32 [2048, 2048], P('sp', 'tp')
- input_grad: bfloat16 [16384, 2048], P('sp')
- recur_grad: bfloat16 [16384, 2048], P('sp', 'tp')
- gate_grad: bfloat16 [16384, 2048], P('sp', 'tp')
The draws below stay inside these ranges and needn't reach their ends.
Inputs may be any that keep to these rules, and one draw needn't show every extreme that they name: `expert_ids`: within each aligned block of 256 tokens a token names 2 different experts, and no expert is named more than 16 times.
All inputs are finite; a program needn't handle non-finite values.
Results may differ from the reference program's by a relative error of at most 0.012.
Values may be sent and summed in bfloat16 or wider, within the bound.
A program may use at most 128 MiB of HBM per device.

```python
import math
import jax
import jax.numpy as jnp
import numpy as np
from jax import lax

D = 2048
FF = 1024
RECURRENCE_WIDTH = 2048
LRU_BLOCKS = 16
TOPK = 2
TOK_DEV = 256
BLK = 128
SEQUENCE_TOKENS = 16384
EXPERTS = 64
CAP = 16
N_SP = 64
N_TP = 2


def decay_parts(key):
    base_key = jax.random.fold_in(key, 4242)
    multiple_count = jax.random.split(base_key, 6)
    fast_share = 0.5
    fast_mask = jax.random.uniform(multiple_count[0], (RECURRENCE_WIDTH,), jnp.float32) < fast_share
    slow_rate = jnp.exp(jax.random.uniform(multiple_count[1], (RECURRENCE_WIDTH,), jnp.float32, math.log(0.03 / SEQUENCE_TOKENS), math.log(0.15 / SEQUENCE_TOKENS)))
    fast_rate = jnp.exp(jax.random.uniform(multiple_count[2], (RECURRENCE_WIDTH,), jnp.float32, math.log(0.0025), math.log(0.008)))
    rate_value = jnp.where(fast_mask, fast_rate, slow_rate)
    block_count = SEQUENCE_TOKENS // TOK_DEV
    factor = jax.random.uniform(multiple_count[3], (block_count, RECURRENCE_WIDTH), jnp.float32, 0.0, 2.0)
    gentle_component = jnp.repeat(-4.0 * rate_value[None, :] * factor, TOK_DEV, axis=0)
    spike_indicator = jax.random.uniform(multiple_count[4], (SEQUENCE_TOKENS, RECURRENCE_WIDTH), jnp.float32) < 3.0 / SEQUENCE_TOKENS
    spike_magnitude = jax.random.uniform(multiple_count[5], (SEQUENCE_TOKENS, RECURRENCE_WIDTH), jnp.float32, 0.22, 0.7)
    additional_value = gentle_component - jnp.where(spike_indicator, spike_magnitude, 0.0)
    return (rate_value, additional_value)


def draw_decay_rate(key, part):
    return decay_parts(key)[0]


def draw_decay_extra(key, part):
    return decay_parts(key)[1]


def with_spikes(drawn, own_key, source, target, blocks, factor):
    def block_of(axis_at):
        return (jnp.arange(drawn.shape[axis_at]) // (drawn.shape[axis_at] // blocks)).reshape((-1,) + (1,) * (drawn.ndim - 1 - axis_at))

    near = jax.random.permutation(own_key, blocks)[block_of(target)]
    second = (block_of(target) + blocks // 2) % blocks
    return jnp.where((block_of(source) == near) | (block_of(source) == second), factor * drawn, drawn)


def levels(key, shape, shards, low, high):
    def one(axis_at, shards_of):
        draws = jax.random.uniform(jax.random.fold_in(jax.random.fold_in(key, 6), axis_at), (shards_of,), jnp.float32, low / len(shards), high / len(shards))
        return jnp.repeat(jnp.exp(draws), shape[axis_at] // shards_of).reshape((-1,) + (1,) * (len(shape) - axis_at - 1))

    loudness = one(*shards[0])
    for cut in shards[1:]:
        loudness = loudness * one(*cut)
    return loudness


def shared_out(own_key, own, number, rows, count, top, limit, lean):
    order = jax.random.permutation(own_key, count)
    heavy_load, ordinary = shares(count, rows * top, limit, lean, True), shares(count, rows * top, limit, lean, False)
    places = jnp.arange(count)

    def named(sizes, turn):
        used = int((sizes > 0).sum())
        fixed = max(1, used // 4)
        passed = fixed + (places - fixed + turn * (used - fixed)) % max(1, count - fixed)
        return jnp.zeros((count,), jnp.int32).at[order[jnp.where(places < fixed, places, passed)]].set(jnp.asarray(sizes, jnp.int32))

    sizes = jnp.where(number % 4 == 0, named(heavy_load, number // 4), named(ordinary, number - number // 4 - 1))
    mixed = jax.random.permutation(jax.random.fold_in(own, 3), count)
    donor, taker = mixed[0:count // 2 * 2:2], mixed[1:count // 2 * 2:2]
    margin = jnp.minimum(sizes[donor] - 1, limit - sizes[taker]) // 2
    margin = jnp.where((donor == order[0]) | (taker == order[0]) | (sizes[taker] == 0), 0, jnp.maximum(margin, 0))
    passed = jax.random.randint(jax.random.fold_in(own, 4), (count // 2,), 0, 1 << 20) % (margin + 1)
    sizes = sizes.at[donor].add(-passed).at[taker].add(passed)
    items = jnp.searchsorted(jnp.cumsum(sizes), jnp.arange(rows * top), side="right").astype(jnp.int32)
    grid = items.reshape(top, rows).T
    grid = grid[jax.random.permutation(jax.random.fold_in(own, 1), rows)]
    turn = jax.random.randint(jax.random.fold_in(own, 2), (rows, 1), 0, top)
    return jnp.take_along_axis(grid, (jnp.arange(top)[None, :] + turn) % top, axis=1)


def shares(amount, total, limit, lean, full):
    loads = [(1 << 20) // math.isqrt(rank ** lean) + 1 for rank in range(1, amount + 1)]
    largest = limit if full else min(limit, max(-(-total // amount), total * loads[0] // sum(loads)))
    least = 1 if total - largest >= amount - 1 else 0
    holding, surplus = [largest] + [least] * (amount - 1), total - largest - least * (amount - 1)
    while surplus > 0:
        free = [i for i in range(1, amount) if holding[i] < largest] or [i for i in range(1, amount) if holding[i] < limit]
        whole, left = sum([loads[i] for i in free]), surplus
        for i in free:
            extra = min(limit - holding[i], max(1, left * loads[i] // whole), surplus)
            holding[i] = holding[i] + extra
            surplus = surplus - extra
    return np.array(holding)


def bell_draw(key, dims, width, reach, cuts=(), kind=jnp.bfloat16):
    entries = width * jax.random.normal(key, dims, jnp.float32)
    if cuts:
        entries = entries * levels(key, dims, cuts, -0.22, 0.18)
    return jnp.clip(entries, -reach, reach).astype(kind)


def heavy_noise(own_key, shape, deviation, most, pieces, heavy, kind=jnp.bfloat16):
    values = deviation * jax.random.normal(own_key, shape, jnp.float32)
    if pieces:
        values = values * levels(own_key, shape, pieces, -0.22, 0.18)
    return jnp.clip(with_spikes(values, jax.random.fold_in(own_key, 3), *heavy), -most, most).astype(kind)


def setup_inputs(seed: int = 0) -> dict:
    keys = jax.random.split(jax.random.key(seed), 17)
    moe_input = bell_draw(keys[0], (SEQUENCE_TOKENS, D), 1.0, 6.0, ((0, 64),))
    cotangent = heavy_noise(keys[1], (SEQUENCE_TOKENS, D), 1.0, 16.0, ((0, 64),), (0, 1, 64, 4.0))
    expert_ids_keys = jax.random.split(jax.random.fold_in(keys[2], 1), SEQUENCE_TOKENS // TOK_DEV)
    expert_ids_turns = jax.random.permutation(jax.random.fold_in(keys[2], 3), SEQUENCE_TOKENS // TOK_DEV)
    expert_ids = jax.vmap(lambda own, number: shared_out(jax.random.fold_in(keys[2], 2), own, number, TOK_DEV, EXPERTS, TOPK, CAP, 1))(expert_ids_keys, expert_ids_turns).reshape((SEQUENCE_TOKENS, TOPK))
    route_weight = jnp.clip(0.05 + 0.55 * jax.random.uniform(keys[3], (SEQUENCE_TOKENS, TOPK), jnp.float32) ** levels(keys[3], (SEQUENCE_TOKENS, TOPK), ((0, 64),), -0.2, 0.2), 0.05, 0.6)
    gate_proj = bell_draw(keys[4], (EXPERTS, D, FF), D ** -0.5, 0.125, ((0, 64), (2, 2)))
    up_proj = bell_draw(keys[5], (EXPERTS, D, FF), D ** -0.5, 0.125, ((0, 64), (2, 2)))
    down_proj = bell_draw(keys[6], (EXPERTS, FF, D), FF ** -0.5, 0.1875, ((0, 64), (1, 2)))
    out_weight = bell_draw(keys[7], (D, RECURRENCE_WIDTH), RECURRENCE_WIDTH ** -0.5, 0.125, ((1, 2),))
    recur_input = bell_draw(keys[8], (SEQUENCE_TOKENS, RECURRENCE_WIDTH), 1.0, 6.0, ((0, 64), (1, 2)))
    gate_input = bell_draw(keys[9], (SEQUENCE_TOKENS, RECURRENCE_WIDTH), 1.0, 6.0, ((0, 64), (1, 2)))
    states = bell_draw(keys[10], (SEQUENCE_TOKENS, RECURRENCE_WIDTH), 1.0, 6.0, ((0, 64), (1, 2)), jnp.float32)
    conv_taps = bell_draw(keys[11], (4, RECURRENCE_WIDTH), 4 ** -0.5, 3.0, ((1, 2),))
    decay_gate_w = bell_draw(keys[12], (LRU_BLOCKS, BLK, BLK), BLK ** -0.5, 0.5, ((0, 2),))
    input_gate_w = bell_draw(keys[13], (LRU_BLOCKS, BLK, BLK), BLK ** -0.5, 0.5, ((0, 2),))
    decay_rate = draw_decay_rate(jax.random.fold_in(keys[16], 71), 0)
    decay_extra = draw_decay_extra(jax.random.fold_in(keys[16], 71), 0)
    return dict(moe_input=moe_input, cotangent=cotangent, expert_ids=expert_ids, route_weight=route_weight, gate_proj=gate_proj, up_proj=up_proj, down_proj=down_proj, out_weight=out_weight, recur_input=recur_input, gate_input=gate_input, states=states, conv_taps=conv_taps, decay_gate_w=decay_gate_w, input_gate_w=input_gate_w, decay_rate=decay_rate, decay_extra=decay_extra)


decay_scale = 8.0

def pair_combine(earlier, later):
    return (earlier[0] * later[0], later[0] * earlier[1] + later[1])

def rounded(value):
    return lax.optimization_barrier(value.astype(jnp.bfloat16)).astype(jnp.float32)

def slot_layout(expert_ids):
    source_ids = expert_ids.reshape(N_SP, TOK_DEV * TOPK)
    onehot = (source_ids[:, :, None] == jnp.arange(EXPERTS, dtype=jnp.int32)[None, None, :]).astype(jnp.int32)
    slot_rank = lax.optimization_barrier(jnp.sum((jnp.cumsum(onehot, axis=1) - onehot) * onehot, axis=2))
    sources = jnp.arange(N_SP, dtype=jnp.int32)[:, None]
    target = ((source_ids * N_SP + sources) * CAP + slot_rank).reshape(-1).astype(jnp.int32)
    source_table = jnp.full((EXPERTS * N_SP * CAP,), SEQUENCE_TOKENS * TOPK, jnp.int32)
    source_table = source_table.at[target].set(jnp.arange(SEQUENCE_TOKENS * TOPK, dtype=jnp.int32))
    return (source_table.reshape(EXPERTS, N_SP * CAP), target)

def reference(moe_input, cotangent, expert_ids, route_weight, gate_proj, up_proj, down_proj, out_weight, recur_input, gate_input, states, conv_taps, decay_gate_w, input_gate_w, decay_rate, decay_extra):
    cot_float = cotangent.astype(jnp.float32)
    scaled = (route_weight[:, :, None] * cot_float[:, None, :]).astype(jnp.bfloat16).reshape(SEQUENCE_TOKENS * TOPK, D)
    token_rows = jnp.repeat(moe_input, TOPK, axis=0)
    zero_row = jnp.zeros((1, D), jnp.bfloat16)
    padded_rows = jnp.concatenate([token_rows, zero_row], axis=0)
    padded_cot = jnp.concatenate([scaled, zero_row], axis=0)
    source_table, target = slot_layout(expert_ids)

    def one_expert(inputs):
        slot_index, weight_gate, weight_up, weight_down = inputs
        rows_float = padded_rows[slot_index].astype(jnp.float32)
        cot_rows = padded_cot[slot_index].astype(jnp.float32)
        gate_float = weight_gate.astype(jnp.float32)
        up_float = weight_up.astype(jnp.float32)
        down_float = weight_down.astype(jnp.float32)
        gate_pre = jnp.dot(rows_float, gate_float)
        up_pre = jnp.dot(rows_float, up_float)
        sigmoid_gate = jax.nn.sigmoid(gate_pre)
        silu_gate = gate_pre * sigmoid_gate
        hidden = rounded(silu_gate * up_pre)
        down_grad = jnp.dot(hidden.T, cot_rows)
        hidden_grad = jnp.dot(cot_rows, down_float.T)
        gate_pre_grad = rounded(hidden_grad * up_pre * sigmoid_gate * (1.0 + gate_pre * (1.0 - sigmoid_gate)))
        up_pre_grad = rounded(hidden_grad * silu_gate)
        gate_weight_grad = jnp.dot(rows_float.T, gate_pre_grad)
        up_weight_grad = jnp.dot(rows_float.T, up_pre_grad)
        share_size = FF // N_TP
        summed = jnp.zeros((N_SP * CAP, D), jnp.float32)
        for part_index in range(N_TP):
            lower = part_index * share_size
            upper = lower + share_size
            piece_grad = jnp.dot(gate_pre_grad[:, lower:upper], gate_float[:, lower:upper].T) + jnp.dot(up_pre_grad[:, lower:upper], up_float[:, lower:upper].T)
            summed = summed + rounded(piece_grad)
        return (gate_weight_grad.astype(jnp.bfloat16), up_weight_grad.astype(jnp.bfloat16), down_grad.astype(jnp.bfloat16), summed.astype(jnp.bfloat16))
    gate_proj_grad, up_proj_grad, down_proj_grad, slot_grad = lax.map(one_expert, (source_table, gate_proj, up_proj, down_proj))
    gathered = slot_grad.reshape(EXPERTS * N_SP * CAP, D)[target].astype(jnp.float32)
    gathered = gathered.reshape(SEQUENCE_TOKENS, TOPK, D)
    moe_grad = gathered[:, 0]
    for choice_index in range(1, TOPK):
        moe_grad = moe_grad + gathered[:, choice_index]
    input_grad = (moe_grad + cot_float).astype(jnp.bfloat16)
    grad_float = input_grad.astype(jnp.float32)
    gate_float_in = gate_input.astype(jnp.float32)
    gelu_value, gelu_back = jax.vjp(jax.nn.gelu, gate_float_in)
    mixer_out = (states * gelu_value).astype(jnp.bfloat16).astype(jnp.float32)
    out_weight_grad = jnp.dot(grad_float.T, mixer_out)
    mixer_grad = jnp.dot(grad_float, out_weight.astype(jnp.float32))
    gate_grad = gelu_back(mixer_grad * states)[0].astype(jnp.bfloat16)
    state_grad = mixer_grad * gelu_value
    taps = conv_taps.astype(jnp.float32)
    padded_in = jnp.pad(recur_input.astype(jnp.float32), ((3, 0), (0, 0)))
    conv = taps[0] * padded_in[0:SEQUENCE_TOKENS]
    for tap_index in range(1, 4):
        conv = conv + taps[tap_index] * padded_in[tap_index:tap_index + SEQUENCE_TOKENS]
    conv_blocks = rounded(conv).reshape(SEQUENCE_TOKENS, LRU_BLOCKS, BLK)
    decay_w = decay_gate_w.astype(jnp.float32)
    input_w = input_gate_w.astype(jnp.float32)
    decay_pre = jnp.einsum('tbi,bij->tbj', conv_blocks, decay_w).reshape(SEQUENCE_TOKENS, RECURRENCE_WIDTH)
    input_pre = jnp.einsum('tbi,bij->tbj', conv_blocks, input_w).reshape(SEQUENCE_TOKENS, RECURRENCE_WIDTH)
    recur_gate = jax.nn.sigmoid(decay_pre)
    input_gate = jax.nn.sigmoid(input_pre)
    positions = jnp.arange(SEQUENCE_TOKENS, dtype=jnp.int32)
    first_row = (positions == 0)[:, None]
    log_decay = -decay_scale * recur_gate * decay_rate[None, :] + decay_extra
    decay_value = jnp.exp(log_decay)
    mult = jnp.where(first_row, 1.0, jnp.sqrt(-jnp.expm1(2.0 * log_decay)))
    prev_states = jnp.concatenate([jnp.zeros((1, RECURRENCE_WIDTH), jnp.float32), states[:-1]], axis=0)
    next_decay = jnp.concatenate([decay_value[1:], jnp.zeros((1, RECURRENCE_WIDTH), jnp.float32)], axis=0)
    cumul_flip, values_flip = lax.associative_scan(pair_combine, (next_decay[::-1], state_grad[::-1]), axis=0)
    carried_grad = values_flip[::-1]
    log_grad = carried_grad * prev_states * decay_value - jnp.where(first_row, 0.0, carried_grad * input_gate * conv * decay_value * decay_value / mult)
    decay_pre_grad = rounded(log_grad * (-decay_scale * decay_rate[None, :]) * recur_gate * (1.0 - recur_gate))
    input_pre_grad = rounded(carried_grad * mult * conv * input_gate * (1.0 - input_gate))
    conv_grad = carried_grad * mult * input_gate + jnp.einsum('tbj,bij->tbi', decay_pre_grad.reshape(SEQUENCE_TOKENS, LRU_BLOCKS, BLK), decay_w).reshape(SEQUENCE_TOKENS, RECURRENCE_WIDTH) + jnp.einsum('tbj,bij->tbi', input_pre_grad.reshape(SEQUENCE_TOKENS, LRU_BLOCKS, BLK), input_w).reshape(SEQUENCE_TOKENS, RECURRENCE_WIDTH)
    padded_grad = jnp.pad(conv_grad, ((0, 3), (0, 0)))
    recur_float = taps[0] * padded_grad[3:3 + SEQUENCE_TOKENS]
    for tap_index in range(1, 4):
        recur_float = recur_float + taps[tap_index] * padded_grad[3 - tap_index:3 - tap_index + SEQUENCE_TOKENS]
    recur_grad = recur_float.astype(jnp.bfloat16)
    return (gate_proj_grad, up_proj_grad, down_proj_grad, out_weight_grad, input_grad, recur_grad, gate_grad)
```

```python
import jax
import jax.numpy as jnp
from jax import lax
from jax.experimental import pallas as pl
from jax.experimental.pallas import tpu as pltpu
from jax.sharding import Mesh
from jax.sharding import PartitionSpec as P

SP = ("sp_0", "sp_1", "sp_2")


MESH = pl.DeviceIdType.MESH


def in_one_piece(arrays, axis, split_dim, concat_dim, along):
    both = jnp.concatenate(arrays, axis=along)
    result, at, outs = (
        lax.all_to_all(both, axis, split_axis=split_dim, concat_axis=concat_dim, tiled=True),
        0,
        [],
    )
    for a in arrays:
        outs.append(lax.slice_in_dim(result, at, at + a.shape[along], axis=along))
        at += a.shape[along]
    return tuple(outs)


def side_by_side(arrays, axis, dim, along):
    ends, at = ([], 0)
    for a in arrays[:-1]:
        at += a.shape[along]
        ends.append(at)
    both = jnp.concatenate(arrays, axis=along)
    return tuple(jnp.split(lax.all_gather(both, axis, axis=dim, tiled=True), ends, axis=along))


def split_up(shard, dim, peers):
    dims = shard.shape
    blocks = shard.reshape(*dims[:dim], peers, dims[dim] // peers, *dims[dim + 1 :])
    return jnp.moveaxis(blocks, dim, 0)


def sum_at_owner(shard, axis, dim):
    peers = lax.axis_size(axis)
    blocks = lax.all_to_all(split_up(shard, dim, peers), axis, 0, 0, tiled=True)
    return jnp.sum(blocks.astype(jnp.float32), axis=0)


def contract_rows(left, right):
    return lax.dot_general(
        left, right, (((0,), (0,)), ((), ())), preferred_element_type=jnp.float32
    )


def contract_cols(left, right):
    return lax.dot_general(
        left, right, (((1,), (1,)), ((), ())), preferred_element_type=jnp.float32
    )


TOK = 256
CH = 1024
LANES = 128
NBLK = 8
ROWS = 64
PARTS = ((0, 384), (384, 384), (768, 256))


def place():
    z, y, x = [lax.axis_index(a) for a in SP]
    return z, y, x, lax.axis_index("tp")


def peer_at(number, core):
    return (number // 16, lax.rem(number // 4, 4), lax.rem(number, 4), core)


def turned(coord, step):
    return lax.rem(coord + step, 4)


def greet_all(me, core, others):
    barrier = pltpu.get_barrier_semaphore()

    def greet(p, carry):
        pl.semaphore_signal(
            barrier, inc=1, device_id=peer_at(lax.rem(me + p, 64), core), device_id_type=MESH
        )
        return carry

    lax.fori_loop(1, 64, greet, 0)
    if others:
        z, y, x, _ = place()
        pl.semaphore_signal(barrier, inc=1, device_id=(z, y, x, 1 - core), device_id_type=MESH)
    return barrier


def gelu_parts(v):
    c = 0.7978845608028654
    inner = c * (v + 0.044715 * v * v * v)
    t = jnp.tanh(inner)
    half = 0.5 * (1.0 + t)
    slope = half + 0.5 * v * (1.0 - t * t) * (c * (1.0 + 3.0 * 0.044715 * v * v))
    return v * half, slope


def minus_expm1(u):
    series = 1.0 + u * (1.0 / 8.0)
    for n in (7, 6, 5, 4, 3, 2):
        series = 1.0 + (u * (1.0 / n)) * series
    return jnp.where(u > -0.25, -u * series, 1.0 - jnp.exp(u))


def later_rows(a, step, fill):
    shifted = pltpu.roll(a, 8 - step, 0)
    rows = lax.broadcasted_iota(jnp.int32, a.shape, 0)
    return jnp.where(rows < 8 - step, shifted, fill)


def mixer_kernel(
    ig_ref, ow_ref, gi_ref, st_ref, ri_ref, taps_ref, dgw_ref, igw_ref, rate_ref, extra_ref,
    owg_ref, rg_ref, gg_ref,
    ext, hin, hst, cv, rgate, igate, dec, mlt, gvs, gds, mo, cum, mg, gext, asend, bsend, aall, ball,
    carry_ref, wbuf, r1, s1, r2, s2, r3,
    hs, hr, a_s, a_r, b_s, b_r, g_s, g_r, w1s, w1r, w2s, w2r, w3s, w3r,
):
    z, y, x, core = place()
    me = (z * 4 + y) * 4 + x
    f32 = jnp.float32
    barrier = greet_all(me, core, False)
    pl.semaphore_wait(barrier, 63)
    after = peer_at(lax.rem(me + 1, 64), core)
    before = peer_at(lax.rem(me + 63, 64), core)

    halo = [
        pltpu.make_async_remote_copy(
            ri_ref.at[pl.ds(TOK - 8, 8)], hin, hs.at[0], hr.at[0], device_id=after, device_id_type=MESH
        ),
        pltpu.make_async_remote_copy(
            st_ref.at[pl.ds(TOK - 8, 8)], hst, hs.at[1], hr.at[1], device_id=after, device_id_type=MESH
        ),
    ]
    for copy in halo:
        copy.start()
    ext[8:] = ri_ref[...].astype(f32)
    for copy in halo:
        copy.wait()
    start = me > 0
    ext[:8] = jnp.where(start, hin[...].astype(f32), 0.0)

    def before_rows(block, carry):
        cols = pl.ds(pl.multiple_of(block * LANES, LANES), LANES)
        taps = taps_ref[:, cols].astype(f32)
        rate = rate_ref[:, cols]
        for r0 in range(0, TOK, ROWS):
            rows = slice(r0, r0 + ROWS)
            conv = taps[0:1] * ext[5 + r0 : 5 + r0 + ROWS, cols]
            for k in range(1, 4):
                conv = conv + taps[k : k + 1] * ext[5 + k + r0 : 5 + k + r0 + ROWS, cols]
            cb = conv.astype(jnp.bfloat16)
            dgate = jax.nn.sigmoid(jnp.dot(cb, dgw_ref[block], preferred_element_type=f32))
            igt = jax.nn.sigmoid(jnp.dot(cb, igw_ref[block], preferred_element_type=f32))
            ld = -8.0 * dgate * rate + extra_ref[rows, cols]
            m = jnp.sqrt(minus_expm1(2.0 * ld))
            if r0 == 0:
                pos = lax.broadcasted_iota(jnp.int32, m.shape, 0) + me
                m = jnp.where(pos == 0, 1.0, m)
            cv[rows, cols] = conv
            rgate[rows, cols] = dgate
            igate[rows, cols] = igt
            dec[rows, cols] = jnp.exp(ld)
            mlt[rows, cols] = m
            gv, gd = gelu_parts(gi_ref[rows, cols].astype(f32))
            gvs[rows, cols] = gv
            gds[rows, cols] = gd
            mo[rows, cols] = (st_ref[rows, cols] * gv).astype(jnp.bfloat16)
        return carry

    lax.fori_loop(0, NBLK, before_rows, 0)
    dec[TOK:] = jnp.ones((8, CH), f32)

    def next_decay(at):
        own = dec[pl.ds(at, 8), :]
        nxt = dec[pl.ds(at + 8, 8), :]
        rows = lax.broadcasted_iota(jnp.int32, own.shape, 0)
        return jnp.where(rows < 7, pltpu.roll(own, 7, 0), jnp.broadcast_to(nxt[0:1], own.shape))

    def products(n, last):
        at = pl.multiple_of((TOK // 8 - 1 - n) * 8, 8)
        a = next_decay(at)
        for step in (1, 2, 4):
            a = a * later_rows(a, step, 1.0)
        a = a * last
        cum[pl.ds(at, 8), :] = a
        return a[0:1]

    total = lax.fori_loop(0, TOK // 8, products, jnp.ones((1, CH), f32))
    total = total * dec[0:1, :]
    for b in range(NBLK):
        asend[b : b + 1, :] = total[:, b * LANES : (b + 1) * LANES]

    def to_all(src, dst, ssem, rsem, begin):
        def one(p, carry):
            where = lax.rem(me + p, 64)
            if begin:
                slot, target = me, where
            else:
                slot, target = lax.rem(me + 64 - p, 64), where
            copy = pltpu.make_async_remote_copy(
                src, dst.at[slot], ssem.at[p - 1], rsem.at[p - 1],
                device_id=peer_at(target, core), device_id_type=MESH,
            )
            if begin:
                copy.start()
            else:
                copy.wait()
            return carry

        lax.fori_loop(1, 64, one, 0)

    to_all(asend, aall, a_s, a_r, True)

    def project(i, carry):
        left = ig_ref[:, pl.ds(pl.multiple_of(i * 256, 256), 256)]
        res = lax.dot_general(left, mo[...], (((0,), (0,)), ((), ())), preferred_element_type=f32)
        res = res.astype(jnp.bfloat16).reshape(2, 4, 32, CH)
        wbuf[i // 2, pl.ds(2 * lax.rem(i, 2), 2)] = res
        return carry

    lax.fori_loop(0, 8, project, 0)

    def at_axis(axis, d):
        here = [z, y, x]
        here[axis] = turned(here[axis], d)
        return (*here, core)

    first, second, third = (0, 1, 2), (1, 2, 0), (2, 0, 1)
    own = (z, y, x)

    def cut(ref, dim, index, c0, w):
        lead = ref.ndim - 2
        spot = tuple(index if k == dim else slice(None) for k in range(lead))
        return (*spot, slice(None), pl.ds(c0, w))

    def dims_left(part):
        return [a for a in range(3) if a != first[part]]

    def stage1(part, d):
        c0, w = PARTS[part]
        a = first[part]
        return pltpu.make_async_remote_copy(
            wbuf.at[cut(wbuf, a, turned(own[a], d), c0, w)],
            r1.at[d - 1, :, :, :, pl.ds(c0, w)],
            w1s.at[part, d - 1], w1r.at[part, d - 1],
            device_id=at_axis(a, d), device_id_type=MESH,
        )

    def stage2(part, d):
        c0, w = PARTS[part]
        a = second[part]
        return pltpu.make_async_remote_copy(
            s1.at[cut(s1, dims_left(part).index(a), turned(own[a], d), c0, w)],
            r2.at[d - 1, :, :, pl.ds(c0, w)],
            w2s.at[part, d - 1], w2r.at[part, d - 1],
            device_id=at_axis(a, d), device_id_type=MESH,
        )

    def stage3(part, d):
        c0, w = PARTS[part]
        a = third[part]
        return pltpu.make_async_remote_copy(
            s2.at[cut(s2, 0, turned(own[a], d), c0, w)],
            r3.at[d - 1, :, pl.ds(c0, w)],
            w3s.at[part, d - 1], w3r.at[part, d - 1],
            device_id=at_axis(a, d), device_id_type=MESH,
        )

    for d in (2, 1, 3):
        for part in range(3):
            stage1(part, d).start()

    def mix(i, carry):
        cols = pl.ds(pl.multiple_of(i * 256, 256), 256)
        res = jnp.dot(ig_ref[...], ow_ref[:, cols], preferred_element_type=f32)
        gg_ref[:, cols] = (res * st_ref[:, cols] * gds[:, cols]).astype(jnp.bfloat16)
        mg[:, cols] = res * gvs[:, cols]
        return carry

    lax.fori_loop(0, 4, mix, 0)

    def local_tile(n, last):
        at = pl.multiple_of((TOK // 8 - 1 - n) * 8, 8)
        a, b = next_decay(at), mg[pl.ds(at, 8), :]
        for step in (1, 2, 4):
            b = b + a * later_rows(b, step, 0.0)
            a = a * later_rows(a, step, 1.0)
        b = b + a * last
        mg[pl.ds(at, 8), :] = b
        return b[0:1]

    head = lax.fori_loop(0, TOK // 8, local_tile, jnp.zeros((1, CH), f32))
    head = head * dec[0:1, :]
    for b in range(NBLK):
        bsend[b : b + 1, :] = head[:, b * LANES : (b + 1) * LANES]
    to_all(bsend, ball, b_s, b_r, True)
    to_all(asend, aall, a_s, a_r, False)
    to_all(bsend, ball, b_s, b_r, False)

    aall[me] = asend[...]
    ball[me] = bsend[...]

    def fold(n, carry):
        j = 63 - n
        return jnp.where(j > me, ball[j] + aall[j] * carry, carry)

    carried = lax.fori_loop(0, 64, fold, jnp.zeros((NBLK, LANES), f32))
    for b in range(NBLK):
        carry_ref[:, b * LANES : (b + 1) * LANES] = carried[b : b + 1, :]

    def after_rows(block, carry):
        cols = pl.ds(pl.multiple_of(block * LANES, LANES), LANES)
        rate = rate_ref[:, cols]
        incoming = carry_ref[:, cols]
        for r0 in range(0, TOK, ROWS):
            rows = slice(r0, r0 + ROWS)
            grad = mg[rows, cols] + cum[rows, cols] * incoming
            row = lax.broadcasted_iota(jnp.int32, grad.shape, 0)
            if r0 == 0:
                here = st_ref[rows, cols]
                prev = jnp.where(
                    row == 0,
                    jnp.broadcast_to(jnp.where(start, hst[7:8, cols], 0.0), here.shape),
                    pltpu.roll(here, 1, 0),
                )
            else:
                prev = st_ref[r0 - 1 : r0 - 1 + ROWS, cols]
            decay, m, igt, conv = dec[rows, cols], mlt[rows, cols], igate[rows, cols], cv[rows, cols]
            dgate = rgate[rows, cols]
            gi_conv = grad * igt * conv
            second_term = gi_conv * decay * decay / m
            if r0 == 0:
                second_term = jnp.where(row + me == 0, 0.0, second_term)
            lg = grad * prev * decay - second_term
            dpg = (lg * (-8.0 * rate) * dgate * (1.0 - dgate)).astype(jnp.bfloat16)
            gm = grad * m
            ipg = (gm * conv * igt * (1.0 - igt)).astype(jnp.bfloat16)
            cg = gm * igt
            cg = cg + lax.dot_general(
                dpg, dgw_ref[block], (((1,), (1,)), ((), ())), preferred_element_type=f32
            )
            cg = cg + lax.dot_general(
                ipg, igw_ref[block], (((1,), (1,)), ((), ())), preferred_element_type=f32
            )
            gext[rows, cols] = cg
        return carry

    lax.fori_loop(0, NBLK, after_rows, 0)
    tail = pltpu.make_async_remote_copy(
        gext.at[pl.ds(0, 8)], gext.at[pl.ds(TOK, 8)], g_s, g_r, device_id=before, device_id_type=MESH
    )
    tail.start()

    def sum_first(part):
        c0, w = PARTS[part]
        cols = pl.ds(c0, w)
        a = first[part]
        for d in (1, 2, 3):
            stage1(part, d).wait()

        def one(i, carry):
            spot = [0, 0, 0]
            spot[a] = own[a]
            left = dims_left(part)
            spot[left[0]] = i
            for k in range(4):
                spot[left[1]] = k
                total = wbuf[(*spot, slice(None), cols)].astype(f32)
                for d in range(3):
                    total = total + r1[d, i, k, :, cols].astype(f32)
                s1[i, k, :, cols] = total.astype(jnp.bfloat16)
            return carry

        lax.fori_loop(0, 4, one, 0)
        for d in (2, 1, 3):
            stage2(part, d).start()

    def sum_second(part):
        c0, w = PARTS[part]
        cols = pl.ds(c0, w)
        dim = dims_left(part).index(second[part])
        for d in (1, 2, 3):
            stage2(part, d).wait()
        for k in range(4):
            spot = [k, k]
            spot[dim] = own[second[part]]
            total = s1[(*spot, slice(None), cols)].astype(f32)
            for d in range(3):
                total = total + r2[d, k, :, cols].astype(f32)
            s2[k, :, cols] = total.astype(jnp.bfloat16)
        for d in (2, 1, 3):
            stage3(part, d).start()

    def sum_third(part):
        c0, w = PARTS[part]
        cols = pl.ds(c0, w)
        for d in (1, 2, 3):
            stage3(part, d).wait()
        total = s2[(own[third[part]], slice(None), cols)].astype(f32)
        for d in range(3):
            total = total + r3[d, :, cols].astype(f32)
        owg_ref[:, cols] = total

    for part in (2, 0, 1):
        sum_first(part)

    tail.wait()
    gext[TOK:] = jnp.where(me == 63, 0.0, gext[TOK:])

    def last_rows(block, carry):
        cols = pl.ds(pl.multiple_of(block * LANES, LANES), LANES)
        taps = taps_ref[:, cols].astype(f32)
        for r0 in range(0, TOK, ROWS):
            out = taps[0:1] * gext[3 + r0 : 3 + r0 + ROWS, cols]
            for k in range(1, 4):
                out = out + taps[k : k + 1] * gext[3 - k + r0 : 3 - k + r0 + ROWS, cols]
            rg_ref[r0 : r0 + ROWS, cols] = out.astype(jnp.bfloat16)
        return carry

    lax.fori_loop(0, NBLK, last_rows, 0)
    for part in (2, 0, 1):
        sum_second(part)
    for part in (2, 0, 1):
        sum_third(part)


def mixer(input_grad, out_weight, gate_input, states, recur_input, taps, dgw, igw, rate, extra):
    f32, bf16 = jnp.float32, jnp.bfloat16
    vm = pltpu.VMEM
    full = lambda: vm((TOK, CH), f32)
    dma = pltpu.SemaphoreType.DMA
    return pl.pallas_call(
        mixer_kernel,
        out_shape=(
            jax.ShapeDtypeStruct((32, CH), f32),
            jax.ShapeDtypeStruct((TOK, CH), bf16),
            jax.ShapeDtypeStruct((TOK, CH), bf16),
        ),
        in_specs=[pl.BlockSpec(memory_space=vm)] * 10,
        out_specs=[pl.BlockSpec(memory_space=vm)] * 3,
        scratch_shapes=[
            vm((TOK + 8, CH), f32), vm((8, CH), bf16), vm((8, CH), f32),
            full(), full(), full(), vm((TOK + 8, CH), f32), full(), full(), full(),
            vm((TOK, CH), bf16), full(), full(), vm((TOK + 8, CH), f32),
            vm((NBLK, LANES), f32), vm((NBLK, LANES), f32), vm((64, NBLK, LANES), f32),
            vm((64, NBLK, LANES), f32), vm((1, CH), f32),
            vm((4, 4, 4, 32, CH), bf16), vm((3, 4, 4, 32, CH), bf16), vm((4, 4, 32, CH), bf16),
            vm((3, 4, 32, CH), bf16), vm((4, 32, CH), bf16), vm((3, 32, CH), bf16),
            dma((2,)), dma((2,)), dma((63,)), dma((63,)), dma((63,)), dma((63,)), dma, dma,
            dma((3, 3)), dma((3, 3)), dma((3, 3)), dma((3, 3)), dma((3, 3)), dma((3, 3)),
        ],
        compiler_params=pltpu.CompilerParams(
            collective_id=1, has_side_effects=True, vmem_limit_bytes=60 * 1024 * 1024
        ),
        name="mixer",
    )(input_grad, out_weight, gate_input, states, recur_input, taps, dgw, igw, rate, extra)


def on_device(
    moe_input,
    cotangent,
    expert_ids,
    route_weight,
    gate_proj,
    up_proj,
    down_proj,
    out_weight,
    recur_input,
    gate_input,
    states,
    conv_taps,
    decay_gate_w,
    input_gate_w,
    decay_rate,
    decay_extra,
):
    experts = lax.axis_size(SP)
    cores = lax.axis_size("tp")
    tok_rows, width = moe_input.shape
    top_count = expert_ids.shape[1]
    capacity = max(2, 4 * tok_rows // experts)
    slot_count = experts * capacity
    flat_ids = expert_ids.reshape(-1)
    onehot = (flat_ids[:, None] == jnp.arange(experts, dtype=jnp.int32)[None, :]).astype(jnp.int32)
    slot_rank = jnp.sum((jnp.cumsum(onehot, axis=0) - onehot) * onehot, axis=1)
    target = flat_ids * capacity + slot_rank
    slot_iota = jnp.arange(slot_count, dtype=jnp.int32)
    placing = (slot_iota[:, None] == target[None, :]).astype(jnp.bfloat16)
    pair_slots = target.reshape(tok_rows, top_count)
    placing_tok = jnp.any(slot_iota[:, None, None] == pair_slots[None, :, :], axis=2).astype(
        jnp.bfloat16
    )
    scaled = (route_weight[:, :, None] * cotangent.astype(jnp.float32)[:, None, :]).astype(
        jnp.bfloat16
    )
    scaled = scaled.reshape(tok_rows * top_count, width)
    send_rows = jnp.dot(placing_tok, moe_input, preferred_element_type=jnp.float32).astype(
        jnp.bfloat16
    )
    send_rows = send_rows.reshape(experts, capacity, width)
    send_grads = jnp.dot(placing, scaled, preferred_element_type=jnp.float32).astype(jnp.bfloat16)
    send_grads = send_grads.reshape(experts, capacity, width)
    share_size = capacity // cores
    offset = lax.axis_index("tp") * share_size
    mine_rows = lax.dynamic_slice_in_dim(send_rows, offset, share_size, 1)
    mine_grads = lax.dynamic_slice_in_dim(send_grads, offset, share_size, 1)
    got_rows, got_grads = in_one_piece((mine_rows, mine_grads), SP, 0, 0, 1)
    arrived_rows, arrived_grads = side_by_side((got_rows, got_grads), "tp", 1, 0)
    rows_in = arrived_rows.reshape(slot_count, width)
    grads_in = arrived_grads.reshape(slot_count, width)
    weight_gate = gate_proj[0]
    weight_up = up_proj[0]
    weight_down = down_proj[0]
    gate_pre = jnp.dot(rows_in, weight_gate, preferred_element_type=jnp.float32)
    up_pre = jnp.dot(rows_in, weight_up, preferred_element_type=jnp.float32)
    sigmoid_gate = jax.nn.sigmoid(gate_pre)
    silu_gate = gate_pre * sigmoid_gate
    hidden = (silu_gate * up_pre).astype(jnp.bfloat16)
    down_grad = contract_rows(hidden, grads_in)
    hidden_grad = contract_cols(grads_in, weight_down)
    gate_pre_grad = (
        hidden_grad * up_pre * sigmoid_gate * (1.0 + gate_pre * (1.0 - sigmoid_gate))
    ).astype(jnp.bfloat16)
    up_pre_grad = (hidden_grad * silu_gate).astype(jnp.bfloat16)
    gate_weight_grad = contract_rows(rows_in, gate_pre_grad)
    up_weight_grad = contract_rows(rows_in, up_pre_grad)
    partial_rows = contract_cols(gate_pre_grad, weight_gate) + contract_cols(up_pre_grad, weight_up)
    shared = sum_at_owner(
        partial_rows.reshape(experts, capacity, width).astype(jnp.bfloat16), "tp", 1
    )
    back_half = lax.all_to_all(
        shared.astype(jnp.bfloat16), SP, split_axis=0, concat_axis=0, tiled=True
    )
    returned = lax.all_gather(back_half, "tp", axis=1, tiled=True)
    moe_grad = contract_rows(placing_tok, returned.reshape(slot_count, width))
    input_grad = (moe_grad + cotangent.astype(jnp.float32)).astype(jnp.bfloat16)
    out_weight_grad, recur_grad, gate_grad = mixer(
        input_grad,
        out_weight,
        gate_input,
        states,
        recur_input,
        conv_taps,
        decay_gate_w,
        input_gate_w,
        decay_rate.reshape(1, -1),
        decay_extra,
    )
    return (
        gate_weight_grad.astype(jnp.bfloat16)[None],
        up_weight_grad.astype(jnp.bfloat16)[None],
        down_grad.astype(jnp.bfloat16)[None],
        out_weight_grad,
        input_grad,
        recur_grad,
        gate_grad,
    )


def solution(mesh):
    finer = Mesh(mesh.devices.reshape(4, 4, 4, mesh.shape["tp"]), ("sp_0", "sp_1", "sp_2", "tp"))
    placed = (
        P(SP, None),
        P(SP, None),
        P(SP, None),
        P(SP, None),
        P(SP, None, "tp"),
        P(SP, None, "tp"),
        P(SP, "tp", None),
        P(None, "tp"),
        P(SP, "tp"),
        P(SP, "tp"),
        P(SP, "tp"),
        P(None, "tp"),
        P("tp", None, None),
        P("tp", None, None),
        P("tp"),
        P(SP, "tp"),
    )
    return jax.shard_map(
        on_device,
        mesh=finer,
        in_specs=placed,
        out_specs=(
            P(SP, None, "tp"),
            P(SP, None, "tp"),
            P(SP, "tp", None),
            P(SP, "tp"),
            P(SP, None),
            P(SP, "tp"),
            P(SP, "tp"),
        ),
        check_vma=False,
    )
```
